32 devices in a mesh: ep: 16 (over z, y, x), tp: 2 (over core).
Axes of the slice: x: 2, y: 2, z: 4, core: 2. Of those that a mesh axis runs over, the one named last changes fastest.
Arguments:
- tokens: bfloat16 [3072, 2048], P('ep', 'tp'), may hold values from -6 to 6
- chosen: int32 [16, 384], P('ep'), may hold values from 0 to 3071, as said below
- gate_score: float32 [16, 384], P('ep'), may hold values from 0.1 to 1
- gate_weight: bfloat16 [16, 2048, 2048], P('ep', None, 'tp'), may hold values from -0.125 to 0.125
- up_weight: bfloat16 [16, 2048, 2048], P('ep', None, 'tp'), may hold values from -0.125 to 0.125
- down_weight: bfloat16 [16, 2048, 2048], P('ep', 'tp'), may hold values from -0.125 to 0.125
Outputs:
- mixed: bfloat16 [3072, 2048], P('ep', 'tp')
The draws below stay inside these ranges and needn't reach their ends.
Inputs may be any that keep to these rules, and one draw needn't show every extreme that they name: For every expert and every s, columns s * 24 to (s + 1) * 24 - 1 of chosen name 24 different tokens, all among tokens s * 192 to (s + 1) * 192 - 1.
All inputs are finite; a program needn't handle non-finite values.
Results may differ from the reference program's by a relative error of at most 0.012.
Values may be sent and summed in bfloat16 or wider, within the bound.
No kernel may reach another device: no remote copies, remote signals or barrier semaphores. Data moves between devices by JAX's collectives and lax.ppermute only.
A program may use at most 128 MiB of HBM per device.

```python
import math
import jax
import jax.numpy as jnp
from jax import lax

D = 2048
FF = 2048
TOK_DEV = 192
PICK = 24
EXPERTS = 16
TOKENS = 3072
CAP = 384
N_TP = 2


def draw_chosen(key, part):
    all_keys = jax.random.split(key, EXPERTS * EXPERTS)
    drawn = jax.vmap(lambda k: jax.random.permutation(k, TOK_DEV)[:PICK])(all_keys)
    drawn = drawn.reshape(EXPERTS, EXPERTS, PICK).astype(jnp.int32)
    block_start = (jnp.arange(EXPERTS, dtype=jnp.int32) * TOK_DEV)[None, :, None]
    return (drawn + block_start).reshape(EXPERTS, CAP).astype(jnp.int32)


def steps_of(own_key, shape, pieces, least, largest):
    gain = 1.0
    for dim, blocks in pieces:
        draws = jax.random.uniform(jax.random.fold_in(jax.random.fold_in(own_key, 6), dim), (blocks,), jnp.float32, least / len(pieces), largest / len(pieces))
        gain = gain * jnp.repeat(jnp.exp(draws), shape[dim] // blocks).reshape((-1,) + (1,) * (len(shape) - 1 - dim))
    return gain


def gaussian(rng, shape, width, bound, cuts=(), kind=jnp.bfloat16):
    values = jax.random.normal(rng, shape, jnp.float32) * width
    if len(cuts) > 0:
        values = steps_of(rng, shape, cuts, -0.22, 0.18) * values
    return jnp.clip(values, min=-bound, max=bound).astype(kind)


def setup_inputs(seed: int = 0) -> dict:
    key_of = jax.random.split(jax.random.key(seed), 7)
    tokens = gaussian(key_of[0], (TOKENS, D), 1.0, 6.0, ((0, 16), (1, 2)))
    chosen = draw_chosen(jax.random.fold_in(key_of[6], 71), 0)
    gate_score = jnp.clip(jnp.exp(math.log(1.0) - 2.3025851 * jax.random.uniform(key_of[2], (EXPERTS, CAP), jnp.float32) ** steps_of(key_of[2], (EXPERTS, CAP), ((0, 16),), -0.2, 0.2)), 0.1, 1.0)
    gate_weight = gaussian(key_of[3], (EXPERTS, D, FF), D ** -0.5, 0.125, ((0, 16), (2, 2)))
    up_weight = gaussian(key_of[4], (EXPERTS, D, FF), D ** -0.5, 0.125, ((0, 16), (2, 2)))
    down_weight = gaussian(key_of[5], (EXPERTS, FF, D), FF ** -0.5, 0.125, ((0, 16), (1, 2)))
    return dict(tokens=tokens, chosen=chosen, gate_score=gate_score, gate_weight=gate_weight, up_weight=up_weight, down_weight=down_weight)


def reference(tokens, chosen, gate_score, gate_weight, up_weight, down_weight):
    ff_part = FF // N_TP

    def expert_step(total, inputs):
        token_ids, scores, w_gate, w_up, w_down = inputs
        picked = jnp.take(tokens, token_ids, axis=0)
        gate_pre = jnp.dot(picked, w_gate, preferred_element_type=jnp.float32)
        up_pre = jnp.dot(picked, w_up, preferred_element_type=jnp.float32)
        hidden = (jax.nn.silu(gate_pre) * up_pre).astype(jnp.bfloat16)
        summed = jnp.zeros((CAP, D), jnp.float32)
        for shard_index in range(N_TP):
            lower = shard_index * ff_part
            partial_value = jnp.dot(hidden[:, lower:lower + ff_part], w_down[lower:lower + ff_part],
                              preferred_element_type=jnp.float32).astype(jnp.bfloat16)
            summed = summed + lax.optimization_barrier(partial_value).astype(jnp.float32)
        weighted = (summed * scores[:, None]).astype(jnp.bfloat16)
        total = total.at[token_ids].add(lax.optimization_barrier(weighted).astype(jnp.float32))
        return total, None

    start_total = jnp.zeros((TOKENS, D), jnp.float32)
    total, _ = lax.scan(expert_step, start_total, (chosen, gate_score, gate_weight, up_weight, down_weight))
    return total.astype(jnp.bfloat16)
```

```python
import jax
import jax.numpy as jnp
from jax import lax
from jax.sharding import PartitionSpec as P


def on_device(tokens, chosen, gate_score, gate_weight, up_weight, down_weight):
    ep_count = lax.axis_size("ep")
    tok_rows, width = tokens.shape
    per_source = chosen.shape[1] // ep_count
    offset = lax.axis_index("ep") * tok_rows
    core = lax.axis_index("tp")
    swap = [(0, 1), (1, 0)]
    w_gate = gate_weight[0]
    w_up = up_weight[0]
    w_down = down_weight[0]
    owned_ids = lax.all_to_all(
        chosen.reshape(ep_count, per_source), "ep", split_axis=0, concat_axis=0, tiled=True
    )
    local_rows = owned_ids.reshape(-1) - offset
    positions = lax.broadcasted_iota(jnp.int32, (1, tok_rows), 1)
    selector = (local_rows[:, None] == positions).astype(jnp.bfloat16)
    outgoing = jnp.dot(selector, tokens, preferred_element_type=jnp.float32).astype(jnp.bfloat16)
    arrived = lax.all_to_all(
        outgoing.reshape(ep_count, per_source, width), "ep", split_axis=0, concat_axis=0, tiled=True
    ).reshape(ep_count * per_source, width)
    other = lax.ppermute(arrived, "tp", swap)
    first = core == 0
    picked = jnp.concatenate(
        [jnp.where(first, arrived, other), jnp.where(first, other, arrived)], axis=1
    )
    gate_pre = jnp.dot(picked, w_gate, preferred_element_type=jnp.float32)
    up_pre = jnp.dot(picked, w_up, preferred_element_type=jnp.float32)
    hidden = (jax.nn.silu(gate_pre) * up_pre).astype(jnp.bfloat16)
    partial = jnp.dot(hidden, w_down, preferred_element_type=jnp.float32).astype(jnp.bfloat16)
    kept = lax.dynamic_slice_in_dim(partial, core * width, width, axis=1)
    sent = lax.dynamic_slice_in_dim(partial, (1 - core) * width, width, axis=1)
    got = lax.ppermute(sent, "tp", swap)
    summed = kept.astype(jnp.float32) + got.astype(jnp.float32)
    weighted = (summed * gate_score[0][:, None]).astype(jnp.bfloat16)
    returned = lax.all_to_all(
        weighted.reshape(ep_count, per_source, width), "ep", split_axis=0, concat_axis=0, tiled=True
    ).reshape(ep_count * per_source, width)
    rows = lax.broadcasted_iota(jnp.int32, (tok_rows, 1), 0)
    gather = (rows == local_rows[None, :]).astype(jnp.bfloat16)
    mixed_out = jnp.dot(gather, returned, preferred_element_type=jnp.float32)
    return mixed_out.astype(jnp.bfloat16)


def solution(mesh):
    in_specs = (
        P("ep", "tp"),
        P("ep", None),
        P("ep", None),
        P("ep", None, "tp"),
        P("ep", None, "tp"),
        P("ep", "tp", None),
    )
    out_specs = P("ep", "tp")
    return jax.shard_map(
        on_device, mesh=mesh, in_specs=in_specs, out_specs=out_specs, check_vma=False
    )
```

```python
import jax
import jax.numpy as jnp
from jax import lax
from jax.experimental import pallas as pl
from jax.experimental.pallas import tpu as pltpu
from jax.sharding import PartitionSpec as P


def tiles_of(count):
    tile = 256 if count % 256 == 0 else count
    return [pl.ds(start, tile) for start in range(0, count, tile)]


def half(ref, which, width):
    return pl.ds(pl.multiple_of(which * width, width), width)


def first_kernel(core_ref, own_ref, gate_hbm, up_hbm, gate_ref, up_ref, gate_buf, up_buf, sems):
    width = own_ref.shape[1]
    rows = half(gate_hbm, core_ref[0], width)
    cols = tiles_of(gate_ref.shape[1])
    pairs = ((gate_hbm, gate_buf), (up_hbm, up_buf))
    copies = [
        [pltpu.make_async_copy(src.at[0, rows, c], buf.at[:, c], sems.at[k, j]) for k, (src, buf) in enumerate(pairs)]
        for j, c in enumerate(cols)
    ]
    for step in copies:
        for copy in step:
            copy.start()
    for c, step in zip(cols, copies):
        for copy, out, buf in zip(step, (gate_ref, up_ref), (gate_buf, up_buf)):
            copy.wait()
            out[:, c] = jnp.dot(own_ref[...], buf[:, c], preferred_element_type=jnp.float32)


def second_kernel(
    core_ref, other_ref, gate_ref, up_ref, gate_hbm, up_hbm, down_hbm, hidden_ref, send_ref, gate_buf, up_buf, down_buf, sems
):
    width = other_ref.shape[1]
    theirs = half(gate_hbm, 1 - core_ref[0], width)
    cols = tiles_of(gate_ref.shape[1])
    outs = tiles_of(width)
    pairs = ((gate_hbm, gate_buf), (up_hbm, up_buf))
    copies = [
        [pltpu.make_async_copy(src.at[0, theirs, c], buf.at[:, c], sems.at[k, j]) for k, (src, buf) in enumerate(pairs)]
        for j, c in enumerate(cols)
    ]
    down_copy = pltpu.make_async_copy(down_hbm.at[0, :, theirs], down_buf, sems.at[2, 0])
    for step in copies:
        for copy in step:
            copy.start()
    down_copy.start()
    for c, (gate_copy, up_copy) in zip(cols, copies):
        gate_copy.wait()
        gate_pre = gate_ref[:, c] + jnp.dot(
            other_ref[...], gate_buf[:, c], preferred_element_type=jnp.float32
        )
        up_copy.wait()
        up_pre = up_ref[:, c] + jnp.dot(
            other_ref[...], up_buf[:, c], preferred_element_type=jnp.float32
        )
        hidden_ref[:, c] = (gate_pre / (1.0 + jnp.exp(-gate_pre)) * up_pre).astype(jnp.bfloat16)
    down_copy.wait()
    for c in outs:
        send_ref[:, c] = jnp.dot(
            hidden_ref[...], down_buf[:, c], preferred_element_type=jnp.float32
        ).astype(jnp.bfloat16)


def third_kernel(core_ref, hidden_ref, down_hbm, keep_ref, down_buf, sems):
    width = keep_ref.shape[1]
    cols = tiles_of(width)
    start = core_ref[0] * width
    copies = []
    for j, c in enumerate(cols):
        at = pl.ds(pl.multiple_of(start + c.start, c.size), c.size)
        copies.append(pltpu.make_async_copy(down_hbm.at[0, :, at], down_buf.at[:, c], sems.at[j]))
    for copy in copies:
        copy.start()
    for c, copy in zip(cols, copies):
        copy.wait()
        keep_ref[:, c] = jnp.dot(
            hidden_ref[...], down_buf[:, c], preferred_element_type=jnp.float32
        )


SMEM = pl.BlockSpec(memory_space=pltpu.SMEM)
VMEM = pl.BlockSpec(memory_space=pltpu.VMEM)
HBM = pl.BlockSpec(memory_space=pltpu.HBM)


def call(body, name, in_specs, outs, scratch, flops, nbytes):
    return pl.pallas_call(
        body,
        out_shape=outs,
        in_specs=in_specs,
        out_specs=tuple(VMEM for _ in outs),
        scratch_shapes=scratch,
        cost_estimate=pl.CostEstimate(flops=flops, bytes_accessed=nbytes, transcendentals=0),
        compiler_params=pltpu.CompilerParams(vmem_limit_bytes=48 << 20),
        name=name,
    )


def first_half(core, own, w_gate, w_up):
    rows, width = own.shape
    hidden = w_gate.shape[2]
    pre = jax.ShapeDtypeStruct((rows, hidden), jnp.float32)
    buf = pltpu.VMEM((width, hidden), jnp.bfloat16)
    sems = pltpu.SemaphoreType.DMA((2, len(tiles_of(hidden))))
    return call(
        first_kernel, "ffn_first", [SMEM, VMEM, HBM, HBM], (pre, pre), [buf, buf, sems],
        4 * rows * width * hidden, 4 * width * hidden,
    )(core, own, w_gate, w_up)


def second_half(core, other, gate_pre, up_pre, w_gate, w_up, w_down):
    rows, width = other.shape
    hidden = w_gate.shape[2]
    buf = pltpu.VMEM((width, hidden), jnp.bfloat16)
    sems = pltpu.SemaphoreType.DMA((3, len(tiles_of(hidden))))
    return call(
        second_kernel, "ffn_second", [SMEM, VMEM, VMEM, VMEM, HBM, HBM, HBM],
        (jax.ShapeDtypeStruct((rows, hidden), jnp.bfloat16), jax.ShapeDtypeStruct((rows, width), jnp.bfloat16)),
        [buf, buf, pltpu.VMEM((hidden, width), jnp.bfloat16), sems],
        6 * rows * width * hidden, 6 * width * hidden,
    )(core, other, gate_pre, up_pre, w_gate, w_up, w_down)


def third_part(core, hidden, w_down, width):
    rows, units = hidden.shape
    return call(
        third_kernel, "ffn_third", [SMEM, VMEM, HBM],
        (jax.ShapeDtypeStruct((rows, width), jnp.float32),),
        [pltpu.VMEM((units, width), jnp.bfloat16), pltpu.SemaphoreType.DMA((len(tiles_of(width)),))],
        2 * rows * width * units, 2 * width * units,
    )(core, hidden, w_down)[0]


def on_device(tokens, chosen, gate_score, gate_weight, up_weight, down_weight):
    ep_count = lax.axis_size("ep")
    tok_rows, width = tokens.shape
    per_source = chosen.shape[1] // ep_count
    offset = lax.axis_index("ep") * tok_rows
    core = lax.axis_index("tp").astype(jnp.int32).reshape(1)
    swap = [(0, 1), (1, 0)]
    owned_ids = lax.all_to_all(
        chosen.reshape(ep_count, per_source), "ep", split_axis=0, concat_axis=0, tiled=True
    )
    local_rows = owned_ids.reshape(-1) - offset
    positions = lax.broadcasted_iota(jnp.int32, (1, tok_rows), 1)
    selector = (local_rows[:, None] == positions).astype(jnp.bfloat16)
    outgoing = jnp.dot(selector, tokens, preferred_element_type=jnp.float32).astype(jnp.bfloat16)
    arrived = lax.all_to_all(
        outgoing.reshape(ep_count, per_source, width), "ep", split_axis=0, concat_axis=0, tiled=True
    ).reshape(ep_count * per_source, width)
    other = lax.ppermute(arrived, "tp", swap)
    gate_pre, up_pre = first_half(core, arrived, gate_weight, up_weight)
    hidden, sent = second_half(core, other, gate_pre, up_pre, gate_weight, up_weight, down_weight)
    got = lax.ppermute(sent, "tp", swap)
    kept = third_part(core, hidden, down_weight, width)
    summed = kept + got.astype(jnp.float32)
    weighted = (summed * gate_score[0][:, None]).astype(jnp.bfloat16)
    returned = lax.all_to_all(
        weighted.reshape(ep_count, per_source, width), "ep", split_axis=0, concat_axis=0, tiled=True
    ).reshape(ep_count * per_source, width)
    rows = lax.broadcasted_iota(jnp.int32, (tok_rows, 1), 0)
    gather = (rows == local_rows[None, :]).astype(jnp.bfloat16)
    mixed_out = jnp.dot(gather, returned, preferred_element_type=jnp.float32)
    return mixed_out.astype(jnp.bfloat16)


def solution(mesh):
    in_specs = (
        P("ep", "tp"),
        P("ep", None),
        P("ep", None),
        P("ep", None, "tp"),
        P("ep", None, "tp"),
        P("ep", "tp", None),
    )
    out_specs = P("ep", "tp")
    return jax.shard_map(
        on_device, mesh=mesh, in_specs=in_specs, out_specs=out_specs, check_vma=False
    )
```

```python
import jax
import jax.numpy as jnp
from jax import lax
from jax.experimental import pallas as pl
from jax.experimental.pallas import tpu as pltpu
from jax.sharding import PartitionSpec as P

SMEM = pl.BlockSpec(memory_space=pltpu.SMEM)
VMEM = pl.BlockSpec(memory_space=pltpu.VMEM)
HBM = pl.BlockSpec(memory_space=pltpu.HBM)
MIB = 1 << 20


def nbytes(x):
    return x.size * x.dtype.itemsize


def call(body, name, in_specs, outs, flops, args, scratch=(), grant=0):
    held = sum(nbytes(x) for x in outs)
    held += sum(nbytes(x) for x, spec in zip(args, in_specs) if spec is VMEM)
    return pl.pallas_call(
        body,
        out_shape=outs,
        in_specs=in_specs,
        out_specs=tuple(VMEM for _ in outs),
        scratch_shapes=scratch,
        cost_estimate=pl.CostEstimate(flops=flops, bytes_accessed=held, transcendentals=0),
        compiler_params=pltpu.CompilerParams(
            vmem_limit_bytes=grant or min(held + 6 * MIB, 60 * MIB)
        ),
        name=name,
    )(*args)


def dot(a, b):
    return jnp.dot(a, b, preferred_element_type=jnp.float32)


def half(which, width):
    return pl.ds(pl.multiple_of(which * width, width), width)


def pick_kernel(per_source, place, ids_ref, within_ref, expert_ref, tokens_ref, out_ref, row_ref):
    me = place[0]
    count, slots = ids_ref.shape
    tok_rows = tokens_ref.shape[0]
    local = (ids_ref[...] - me * tok_rows).astype(jnp.float32)
    spread = lax.broadcasted_iota(jnp.int32, (slots, slots), 0) == me * per_source + within_ref[...]
    mine = jnp.dot(
        local, spread.astype(jnp.float32),
        precision=lax.Precision.HIGHEST, preferred_element_type=jnp.float32,
    )
    ours = lax.broadcasted_iota(jnp.int32, (count, slots), 0) == (expert_ref[...] ^ me)
    row = jnp.sum(jnp.where(ours, mine, 0.0), axis=0, keepdims=True).astype(jnp.int32)
    row_ref[...] = row
    selector = lax.broadcasted_iota(jnp.int32, (tok_rows, slots), 0) == row
    out_ref[...] = lax.dot_general(
        selector.astype(jnp.float32).astype(jnp.bfloat16), tokens_ref[...],
        (((0,), (0,)), ((), ())), preferred_element_type=jnp.float32,
    ).astype(jnp.bfloat16)


def first_kernel(place, own_ref, gate_w, up_w, gate_ref, up_ref):
    mine = half(place[1], own_ref.shape[1])
    gate_ref[...] = dot(own_ref[...], gate_w[0, mine, :])
    up_ref[...] = dot(own_ref[...], up_w[0, mine, :])


def scaled(score_ref, value):
    rows, width = value.shape
    column = jnp.transpose(jnp.broadcast_to(score_ref[...], (128, rows)))
    pieces = [value[:, c : c + 128] * column for c in range(0, width, 128)]
    return jnp.concatenate(pieces, axis=1)


def second_kernel(
    place, other_ref, gate_ref, up_ref, gate_w, up_w, down_w, score_ref, hidden_ref, send_ref
):
    theirs = half(1 - place[1], other_ref.shape[1])
    units = gate_ref.shape[1]
    tile = 256 if units % 256 == 0 else units
    for start in range(0, units, tile):
        c = pl.ds(start, tile)
        gate_pre = gate_ref[:, c] + dot(other_ref[...], gate_w[0, theirs, c])
        up_pre = up_ref[:, c] + dot(other_ref[...], up_w[0, theirs, c])
        hidden_ref[:, c] = (gate_pre / (1.0 + jnp.exp(-gate_pre)) * up_pre).astype(jnp.bfloat16)
    send_ref[...] = scaled(score_ref, dot(hidden_ref[...], down_w[0, :, theirs])).astype(jnp.bfloat16)


def third_kernel(place, hidden_ref, down_w, score_ref, keep_ref):
    mine = half(place[1], keep_ref.shape[1])
    keep_ref[...] = scaled(score_ref, dot(hidden_ref[...], down_w[0, :, mine]))


def mix_kernel(row_ref, returned_ref, out_ref):
    shape = (out_ref.shape[0], row_ref.shape[1])
    selector = lax.broadcasted_iota(jnp.int32, shape, 0) == row_ref[...]
    out_ref[...] = dot(
        selector.astype(jnp.float32).astype(jnp.bfloat16), returned_ref[...]
    ).astype(out_ref.dtype)


def gather_round(value, stride, radix, count):
    parts = [value]
    for k in range(1, radix):
        parts.append(lax.ppermute(value, "ep", [(e, e ^ (k * stride)) for e in range(count)]))
    return parts


def on_device(tokens, chosen, gate_score, gate_weight, up_weight, down_weight):
    ep_count = lax.axis_size("ep")
    tok_rows, width = tokens.shape
    slots = chosen.shape[1]
    per_source = slots // ep_count
    rows = ep_count * per_source
    units = gate_weight.shape[2]
    me = lax.axis_index("ep").astype(jnp.int32)
    place = jnp.stack([me, lax.axis_index("tp").astype(jnp.int32)])
    swap = [(0, 1), (1, 0)]

    ids, stride = chosen, 1
    while stride < ep_count:
        radix = 4 if ep_count % (4 * stride) == 0 else 2
        ids = jnp.concatenate(gather_round(ids, stride, radix, ep_count), axis=0)
        stride *= radix

    order = jnp.arange(slots, dtype=jnp.int32)[None, :]
    outgoing, row = call(
        lambda *refs: pick_kernel(per_source, *refs), "pick", [SMEM] + [VMEM] * 4,
        (
            jax.ShapeDtypeStruct((rows, width), tokens.dtype),
            jax.ShapeDtypeStruct((1, slots), jnp.int32),
        ),
        200 * rows * tok_rows * width,
        (place, ids, order % per_source, order // per_source, tokens),
        (), 0 if rows < 1024 else 48 * MIB,
    )
    arrived = lax.all_to_all(
        outgoing.reshape(ep_count, per_source, width), "ep", split_axis=0, concat_axis=0, tiled=True
    ).reshape(rows, width)
    other = lax.ppermute(arrived, "tp", swap)
    pre = jax.ShapeDtypeStruct((rows, units), jnp.float32)
    product = 2 * rows * width * units
    gate_pre, up_pre = call(
        first_kernel, "ffn_first", [SMEM] + [VMEM] * 3, (pre, pre), 2 * product,
        (place, arrived, gate_weight, up_weight),
    )
    hidden, sent = call(
        second_kernel, "ffn_second", [SMEM] + [VMEM] * 7,
        (
            jax.ShapeDtypeStruct((rows, units), jnp.bfloat16),
            jax.ShapeDtypeStruct((rows, width), jnp.bfloat16),
        ),
        3 * product,
        (place, other, gate_pre, up_pre, gate_weight, up_weight, down_weight, gate_score),
    )
    got = lax.ppermute(sent, "tp", swap)
    (kept,) = call(
        third_kernel, "ffn_third", [SMEM] + [VMEM] * 3,
        (jax.ShapeDtypeStruct((rows, width), jnp.float32),), product,
        (place, hidden, down_weight, gate_score),
    )
    weighted = (kept + got.astype(jnp.float32)).astype(jnp.bfloat16)
    returned = lax.all_to_all(
        weighted.reshape(ep_count, per_source, width), "ep", split_axis=0, concat_axis=0, tiled=True
    ).reshape(rows, width)
    (mixed_out,) = call(
        mix_kernel, "mix", [VMEM] * 2, (jax.ShapeDtypeStruct((tok_rows, width), jnp.bfloat16),),
        2 * rows * tok_rows * width, (row, returned),
    )
    return mixed_out


def solution(mesh):
    in_specs = (
        P("ep", "tp"),
        P("ep", None),
        P("ep", None),
        P("ep", None, "tp"),
        P("ep", None, "tp"),
        P("ep", "tp", None),
    )
    out_specs = P("ep", "tp")
    return jax.shard_map(
        on_device, mesh=mesh, in_specs=in_specs, out_specs=out_specs, check_vma=False
    )
```

```python
import jax
import jax.numpy as jnp
from jax import lax
from jax.experimental import pallas as pl
from jax.experimental.pallas import tpu as pltpu
from jax.sharding import PartitionSpec as P

SMEM = pl.BlockSpec(memory_space=pltpu.SMEM)
VMEM = pl.BlockSpec(memory_space=pltpu.VMEM)
HBM = pl.BlockSpec(memory_space=pltpu.HBM)
MIB = 1 << 20


def nbytes(x):
    return x.size * x.dtype.itemsize


def call(body, name, in_specs, outs, flops, args, scratch=(), grant=0):
    held = sum(nbytes(x) for x in outs)
    held += sum(nbytes(x) for x, spec in zip(args, in_specs) if spec is VMEM)
    return pl.pallas_call(
        body,
        out_shape=outs,
        in_specs=in_specs,
        out_specs=tuple(VMEM for _ in outs),
        scratch_shapes=scratch,
        cost_estimate=pl.CostEstimate(flops=flops, bytes_accessed=held, transcendentals=0),
        compiler_params=pltpu.CompilerParams(
            vmem_limit_bytes=grant or min(held + 6 * MIB, 60 * MIB)
        ),
        name=name,
    )(*args)


def dot(a, b):
    return jnp.dot(a, b, preferred_element_type=jnp.float32)


def half(which, width):
    return pl.ds(pl.multiple_of(which * width, width), width)


def prep_kernel(per_source, place, within_ref, spread_ref):
    slots = within_ref.shape[1]
    column = lax.broadcasted_iota(jnp.int32, (slots, slots), 0)
    hit = column == place[0] * per_source + within_ref[...]
    spread_ref[...] = hit.astype(jnp.float32).astype(jnp.bfloat16)


def pick_kernel(place, expert_ref, spread_ref, tokens_ref, *refs):
    parts, (out_ref, row_ref, ids_ref) = refs[:-3], refs[-3:]
    me = place[0]
    tok_rows, slots = tokens_ref.shape[0], spread_ref.shape[0]
    step = parts[0].shape[0]
    count = step * len(parts)
    for j, part in enumerate(parts):
        ids_ref[pl.ds(j * step, step), :] = part[...]
    local = ids_ref[...] - me * tok_rows
    low, high = local & 127, local >> 7
    both = jnp.concatenate([high, low], axis=0).astype(jnp.float32).astype(jnp.bfloat16)
    mine = dot(both, spread_ref[...])
    mine = mine[:count] * 128.0 + mine[count:]
    ours = lax.broadcasted_iota(jnp.int32, (count, slots), 0) == (expert_ref[...] ^ me)
    row = jnp.sum(jnp.where(ours, mine, 0.0), axis=0, keepdims=True).astype(jnp.int32)
    row_ref[...] = row
    selector = lax.broadcasted_iota(jnp.int32, (tok_rows, slots), 0) == row
    out_ref[...] = lax.dot_general(
        selector.astype(jnp.float32).astype(jnp.bfloat16), tokens_ref[...],
        (((0,), (0,)), ((), ())), preferred_element_type=jnp.float32,
    ).astype(jnp.bfloat16)


def first_kernel(place, own_ref, gate_w, up_w, gate_ref, up_ref):
    mine = half(place[1], own_ref.shape[1])
    gate_ref[...] = dot(own_ref[...], gate_w[0, mine, :])
    up_ref[...] = dot(own_ref[...], up_w[0, mine, :])


def second_kernel(
    place, other_ref, gate_ref, up_ref, gate_w, up_w, down_w, score_ref, hidden_ref, send_ref
):
    theirs = half(1 - place[1], other_ref.shape[1])
    rows, units = gate_ref.shape
    tile = 256 if units % 256 == 0 else units
    score = jnp.transpose(jnp.broadcast_to(score_ref[...], (128, rows)))
    score = jnp.concatenate([score] * (tile // 128), axis=1)
    for start in range(0, units, tile):
        c = pl.ds(start, tile)
        gate_pre = gate_ref[:, c] + dot(other_ref[...], gate_w[0, theirs, c])
        up_pre = up_ref[:, c] + dot(other_ref[...], up_w[0, theirs, c])
        hidden = gate_pre / (1.0 + jnp.exp(-gate_pre)) * (up_pre * score)
        hidden_ref[:, c] = hidden.astype(jnp.bfloat16)
    send_ref[...] = dot(hidden_ref[...], down_w[0, :, theirs]).astype(jnp.bfloat16)


def third_kernel(place, hidden_ref, down_w, keep_ref):
    keep_ref[...] = dot(hidden_ref[...], down_w[0, :, half(place[1], keep_ref.shape[1])])


def mix_kernel(row_ref, returned_ref, out_ref):
    shape = (out_ref.shape[0], row_ref.shape[1])
    selector = lax.broadcasted_iota(jnp.int32, shape, 0) == row_ref[...]
    out_ref[...] = dot(
        selector.astype(jnp.float32).astype(jnp.bfloat16), returned_ref[...]
    ).astype(out_ref.dtype)


def gather_round(value, stride, radix, count):
    parts = [value]
    for k in range(1, radix):
        parts.append(lax.ppermute(value, "ep", [(e, e ^ (k * stride)) for e in range(count)]))
    return parts


def on_device(tokens, chosen, gate_score, gate_weight, up_weight, down_weight):
    ep_count = lax.axis_size("ep")
    tok_rows, width = tokens.shape
    slots = chosen.shape[1]
    per_source = slots // ep_count
    rows = ep_count * per_source
    units = gate_weight.shape[2]
    me = lax.axis_index("ep").astype(jnp.int32)
    place = jnp.stack([me, lax.axis_index("tp").astype(jnp.int32)])
    swap = [(0, 1), (1, 0)]

    order = jnp.arange(slots, dtype=jnp.int32)[None, :]
    (spread,) = call(
        lambda *refs: prep_kernel(per_source, *refs), "prep", [SMEM, VMEM],
        (jax.ShapeDtypeStruct((slots, slots), jnp.bfloat16),), 10**10, (place, order % per_source),
    )
    parts, stride = [chosen], 1
    while stride < ep_count:
        ids = jnp.concatenate(parts, axis=0)
        radix = 4 if ep_count % (4 * stride) == 0 else 2
        parts = gather_round(ids, stride, radix, ep_count)
        if stride == 1:
            parts, spread = lax.optimization_barrier((parts, spread))
        stride *= radix

    outgoing, row = call(
        pick_kernel, "pick", [SMEM] + [VMEM] * (3 + len(parts)),
        (
            jax.ShapeDtypeStruct((rows, width), tokens.dtype),
            jax.ShapeDtypeStruct((1, slots), jnp.int32),
        ),
        200 * rows * tok_rows * width,
        (place, order // per_source, spread, tokens, *parts),
        [pltpu.VMEM((ep_count, slots), jnp.int32)],
    )
    arrived = lax.all_to_all(
        outgoing.reshape(ep_count, per_source, width), "ep", split_axis=0, concat_axis=0, tiled=True
    ).reshape(rows, width)
    other = lax.ppermute(arrived, "tp", swap)
    pre = jax.ShapeDtypeStruct((rows, units), jnp.float32)
    product = 2 * rows * width * units
    gate_pre, up_pre = call(
        first_kernel, "ffn_first", [SMEM] + [VMEM] * 3, (pre, pre), 2 * product,
        (place, arrived, gate_weight, up_weight),
    )
    hidden, sent = call(
        second_kernel, "ffn_second", [SMEM] + [VMEM] * 7,
        (
            jax.ShapeDtypeStruct((rows, units), jnp.bfloat16),
            jax.ShapeDtypeStruct((rows, width), jnp.bfloat16),
        ),
        3 * product,
        (place, other, gate_pre, up_pre, gate_weight, up_weight, down_weight, gate_score),
    )
    got = lax.ppermute(sent, "tp", swap)
    (kept,) = call(
        third_kernel, "ffn_third", [SMEM] + [VMEM] * 2,
        (jax.ShapeDtypeStruct((rows, width), jnp.float32),), product,
        (place, hidden, down_weight),
    )
    weighted = (kept + got.astype(jnp.float32)).astype(jnp.bfloat16)
    returned = lax.all_to_all(
        weighted.reshape(ep_count, per_source, width), "ep", split_axis=0, concat_axis=0, tiled=True
    ).reshape(rows, width)
    (mixed_out,) = call(
        mix_kernel, "mix", [VMEM] * 2, (jax.ShapeDtypeStruct((tok_rows, width), jnp.bfloat16),),
        2 * rows * tok_rows * width, (row, returned),
    )
    return mixed_out


def solution(mesh):
    in_specs = (
        P("ep", "tp"),
        P("ep", None),
        P("ep", None),
        P("ep", None, "tp"),
        P("ep", None, "tp"),
        P("ep", "tp", None),
    )
    out_specs = P("ep", "tp")
    return jax.shard_map(
        on_device, mesh=mesh, in_specs=in_specs, out_specs=out_specs, check_vma=False
    )
```

```python
import jax
import jax.numpy as jnp
from jax import lax
from jax.experimental import pallas as pl
from jax.experimental.pallas import tpu as pltpu
from jax.sharding import PartitionSpec as P

VMEM = pl.BlockSpec(memory_space=pltpu.VMEM)
HBM = pl.BlockSpec(memory_space=pltpu.HBM)
MIB = 1 << 20


def nbytes(x):
    return x.size * x.dtype.itemsize


def call(body, name, in_specs, outs, flops, args, scratch=(), grant=0):
    held = sum(nbytes(x) for x in outs)
    held += sum(nbytes(x) for x, spec in zip(args, in_specs) if spec is VMEM)
    return pl.pallas_call(
        body,
        out_shape=outs,
        in_specs=in_specs,
        out_specs=tuple(VMEM for _ in outs),
        scratch_shapes=scratch,
        cost_estimate=pl.CostEstimate(flops=flops, bytes_accessed=held, transcendentals=0),
        compiler_params=pltpu.CompilerParams(
            vmem_limit_bytes=grant or min(held + 6 * MIB, 60 * MIB)
        ),
        name=name,
    )(*args)


def dot(a, b):
    return jnp.dot(a, b, preferred_element_type=jnp.float32)


def half(which, width):
    return pl.ds(pl.multiple_of(which * width, width), width)


def prep_kernel(per_source, within_ref, spread_ref):
    slots = within_ref.shape[1]
    column = lax.broadcasted_iota(jnp.int32, (slots, slots), 0)
    hit = column == lax.axis_index("ep") * per_source + within_ref[...]
    spread_ref[...] = hit.astype(jnp.float32).astype(jnp.bfloat16)


def pick_kernel(expert_ref, code_ref, spread_ref, tokens_ref, *refs):
    parts, (out_ref, row_ref, ids_ref) = refs[:-3], refs[-3:]
    me = lax.axis_index("ep")
    tok_rows, slots = tokens_ref.shape[0], spread_ref.shape[0]
    step = parts[0].shape[0]
    count = step * len(parts)
    for j, part in enumerate(parts):
        ids_ref[pl.ds(j * step, step), :] = part[...]
    local = ids_ref[...] - me * tok_rows
    low, high = local & 127, local >> 7
    both = jnp.concatenate([high, low], axis=0).astype(jnp.float32).astype(jnp.bfloat16)
    mine = dot(both, spread_ref[...])
    mine = mine[:count] * 128.0 + mine[count:]
    ours = code_ref[...] == (expert_ref[...] ^ me)
    row = jnp.sum(jnp.where(ours, mine, 0.0), axis=0, keepdims=True).astype(jnp.int32)
    row_ref[...] = row
    selector = lax.broadcasted_iota(jnp.int32, (tok_rows, slots), 0) == row
    out_ref[...] = lax.dot_general(
        selector.astype(jnp.float32).astype(jnp.bfloat16), tokens_ref[...],
        (((0,), (0,)), ((), ())), preferred_element_type=jnp.float32,
    ).astype(jnp.bfloat16)


def first_kernel(own_ref, gate_w, up_w, down_w, gate_ref, up_ref):
    del down_w
    mine = half(lax.axis_index("tp"), own_ref.shape[1])
    gate_ref[...] = dot(own_ref[...], gate_w[0, mine, :])
    up_ref[...] = dot(own_ref[...], up_w[0, mine, :])


def second_kernel(
    other_ref, gate_ref, up_ref, gate_w, up_w, down_w, score_ref, hidden_ref, send_ref
):
    theirs = half(1 - lax.axis_index("tp"), other_ref.shape[1])
    rows, units = gate_ref.shape
    tile = 512 if units % 512 == 0 else units
    score = jnp.transpose(jnp.broadcast_to(score_ref[...], (128, rows)))
    score = jnp.concatenate([score] * (tile // 128), axis=1)
    for start in range(0, units, tile):
        c = pl.ds(start, tile)
        gate_pre = gate_ref[:, c] + dot(other_ref[...], gate_w[0, theirs, c])
        up_pre = up_ref[:, c] + dot(other_ref[...], up_w[0, theirs, c])
        hidden = gate_pre / (1.0 + jnp.exp(-gate_pre)) * (up_pre * score)
        hidden_ref[:, c] = hidden.astype(jnp.bfloat16)
    send_ref[...] = dot(hidden_ref[...], down_w[0, :, theirs]).astype(jnp.bfloat16)


def third_kernel(hidden_ref, down_w, keep_ref):
    keep_ref[...] = dot(hidden_ref[...], down_w[0, :, half(lax.axis_index("tp"), keep_ref.shape[1])])


def mix_kernel(row_ref, returned_ref, out_ref):
    shape = (out_ref.shape[0], row_ref.shape[1])
    selector = lax.broadcasted_iota(jnp.int32, shape, 0) == row_ref[...]
    out_ref[...] = dot(
        selector.astype(jnp.float32).astype(jnp.bfloat16), returned_ref[...]
    ).astype(out_ref.dtype)


def gather_round(value, stride, radix, count):
    parts = [value]
    for k in range(1, radix):
        parts.append(lax.ppermute(value, "ep", [(e, e ^ (k * stride)) for e in range(count)]))
    return parts


def on_device(tokens, chosen, gate_score, gate_weight, up_weight, down_weight):
    ep_count = lax.axis_size("ep")
    tok_rows, width = tokens.shape
    slots = chosen.shape[1]
    per_source = slots // ep_count
    rows = ep_count * per_source
    units = gate_weight.shape[2]
    swap = [(0, 1), (1, 0)]

    order = jnp.arange(slots, dtype=jnp.int32)[None, :]
    (spread,) = call(
        lambda *refs: prep_kernel(per_source, *refs), "prep", [VMEM],
        (jax.ShapeDtypeStruct((slots, slots), jnp.bfloat16),), 10**10, (order % per_source,),
    )
    parts, codes, stride = [chosen], [0], ep_count
    while stride > 1:
        ids = jnp.concatenate(parts, axis=0)
        radix = 4 if stride % 4 == 0 else 2
        stride //= radix
        codes = [k * stride + c for k in range(radix) for c in codes]
        parts = gather_round(ids, stride, radix, ep_count)
        if stride * radix == ep_count:
            parts, spread = lax.optimization_barrier((parts, spread))

    outgoing, row = call(
        pick_kernel, "pick", [VMEM] * (4 + len(parts)),
        (
            jax.ShapeDtypeStruct((rows, width), tokens.dtype),
            jax.ShapeDtypeStruct((1, slots), jnp.int32),
        ),
        200 * rows * tok_rows * width,
        (order // per_source, jnp.array(codes, jnp.int32)[:, None], spread, tokens, *parts),
        [pltpu.VMEM((ep_count, slots), jnp.int32)],
    )
    arrived = lax.all_to_all(
        outgoing.reshape(ep_count, per_source, width), "ep", split_axis=0, concat_axis=0, tiled=True
    ).reshape(rows, width)
    other = lax.ppermute(arrived, "tp", swap)
    pre = jax.ShapeDtypeStruct((rows, units), jnp.float32)
    product = 2 * rows * width * units
    gate_pre, up_pre = call(
        first_kernel, "ffn_first", [VMEM] * 4, (pre, pre), 2 * product,
        (arrived, gate_weight, up_weight, down_weight),
    )
    hidden, sent = call(
        second_kernel, "ffn_second", [VMEM] * 7,
        (
            jax.ShapeDtypeStruct((rows, units), jnp.bfloat16),
            jax.ShapeDtypeStruct((rows, width), jnp.bfloat16),
        ),
        3 * product,
        (other, gate_pre, up_pre, gate_weight, up_weight, down_weight, gate_score),
    )
    got = lax.ppermute(sent, "tp", swap)
    (kept,) = call(
        third_kernel, "ffn_third", [VMEM] * 2,
        (jax.ShapeDtypeStruct((rows, width), jnp.float32),), product,
        (hidden, down_weight),
    )
    weighted = (kept + got.astype(jnp.float32)).astype(jnp.bfloat16)
    returned = lax.all_to_all(
        weighted.reshape(ep_count, per_source, width), "ep", split_axis=0, concat_axis=0, tiled=True
    ).reshape(rows, width)
    (mixed_out,) = call(
        mix_kernel, "mix", [VMEM] * 2, (jax.ShapeDtypeStruct((tok_rows, width), jnp.bfloat16),),
        2 * rows * tok_rows * width, (row, returned),
    )
    return mixed_out


def solution(mesh):
    in_specs = (
        P("ep", "tp"),
        P("ep", None),
        P("ep", None),
        P("ep", None, "tp"),
        P("ep", None, "tp"),
        P("ep", "tp", None),
    )
    out_specs = P("ep", "tp")
    return jax.shard_map(
        on_device, mesh=mesh, in_specs=in_specs, out_specs=out_specs, check_vma=False
    )
```

```python
import jax
import jax.numpy as jnp
from jax import lax
from jax.experimental import pallas as pl
from jax.experimental.pallas import tpu as pltpu
from jax.sharding import PartitionSpec as P


VMEM = pl.BlockSpec(memory_space=pltpu.VMEM)
HBM = pl.BlockSpec(memory_space=pltpu.HBM)
MIB = 1 << 20


def nbytes(x):
    return x.size * x.dtype.itemsize


def call(body, in_specs, outs, flops, args, scratch=(), grant=0):
    held = sum(nbytes(x) for x in outs)
    held += sum(nbytes(x) for x, spec in zip(args, in_specs) if spec is VMEM)
    return pl.pallas_call(
        body,
        out_shape=outs,
        in_specs=in_specs,
        out_specs=tuple(VMEM for _ in outs),
        scratch_shapes=scratch,
        cost_estimate=pl.CostEstimate(flops=flops, bytes_accessed=held, transcendentals=0),
        compiler_params=pltpu.CompilerParams(
            vmem_limit_bytes=grant or min(held + 6 * MIB, 60 * MIB)
        ),
    )(*args)


def dot(a, b):
    return jnp.dot(a, b, preferred_element_type=jnp.float32)


def half(which, width):
    return pl.ds(pl.multiple_of(which * width, width), width)


def prep_kernel(per_source, within_ref, spread_ref):
    slots = within_ref.shape[1]
    column = lax.broadcasted_iota(jnp.int32, (slots, slots), 0)
    hit = column == lax.axis_index("ep") * per_source + within_ref[...]
    spread_ref[...] = hit.astype(jnp.float32).astype(jnp.bfloat16)


def pick_kernel(expert_ref, code_ref, spread_ref, tokens_ref, *refs):
    parts, (out_ref, row_ref, ids_ref) = refs[:-3], refs[-3:]
    me = lax.axis_index("ep")
    tok_rows, slots = tokens_ref.shape[0], spread_ref.shape[0]
    step = parts[0].shape[0]
    count = step * len(parts)
    for j, part in enumerate(parts):
        ids_ref[pl.ds(j * step, step), :] = part[...]
    local = ids_ref[...] - me * tok_rows
    low, high = local & 127, local >> 7
    both = jnp.concatenate([high, low], axis=0).astype(jnp.float32).astype(jnp.bfloat16)
    mine = dot(both, spread_ref[...])
    mine = mine[:count] * 128.0 + mine[count:]
    ours = code_ref[...] == (expert_ref[...] ^ me)
    row = jnp.sum(jnp.where(ours, mine, 0.0), axis=0, keepdims=True).astype(jnp.int32)
    row_ref[...] = row
    selector = lax.broadcasted_iota(jnp.int32, (tok_rows, slots), 0) == row
    out_ref[...] = lax.dot_general(
        selector.astype(jnp.float32).astype(jnp.bfloat16), tokens_ref[...],
        (((0,), (0,)), ((), ())), preferred_element_type=jnp.float32,
    ).astype(jnp.bfloat16)


def first_kernel(own_ref, gate_w, up_w, down_w, gate_ref, up_ref):
    del down_w
    mine = half(lax.axis_index("tp"), own_ref.shape[1])
    gate_ref[...] = dot(own_ref[...], gate_w[0, mine, :])
    up_ref[...] = dot(own_ref[...], up_w[0, mine, :])


def second_kernel(
    other_ref, gate_ref, up_ref, gate_w, up_w, down_w, score_ref, hidden_ref, send_ref
):
    theirs = half(1 - lax.axis_index("tp"), other_ref.shape[1])
    rows, units = gate_ref.shape
    tile = 512 if units % 512 == 0 else units
    score = jnp.transpose(jnp.broadcast_to(score_ref[...], (128, rows)))
    score = jnp.concatenate([score] * (tile // 128), axis=1)
    for start in range(0, units, tile):
        c = pl.ds(start, tile)
        gate_pre = gate_ref[:, c] + dot(other_ref[...], gate_w[0, theirs, c])
        up_pre = up_ref[:, c] + dot(other_ref[...], up_w[0, theirs, c])
        hidden = gate_pre / (1.0 + jnp.exp(-gate_pre)) * (up_pre * score)
        hidden_ref[:, c] = hidden.astype(jnp.bfloat16)
    send_ref[...] = dot(hidden_ref[...], down_w[0, :, theirs]).astype(jnp.bfloat16)


def third_kernel(hidden_ref, down_w, keep_ref):
    keep_ref[...] = dot(hidden_ref[...], down_w[0, :, half(lax.axis_index("tp"), keep_ref.shape[1])])


def mix_kernel(row_ref, returned_ref, out_ref):
    shape = (out_ref.shape[0], row_ref.shape[1])
    selector = lax.broadcasted_iota(jnp.int32, shape, 0) == row_ref[...]
    out_ref[...] = dot(
        selector.astype(jnp.float32).astype(jnp.bfloat16), returned_ref[...]
    ).astype(out_ref.dtype)


def gather_round(value, stride, radix, count):
    parts = [value]
    for k in range(1, radix):
        parts.append(lax.ppermute(value, "ep", [(e, e ^ (k * stride)) for e in range(count)]))
    return parts


def layer(tokens, chosen, gate_score, gate_weight, up_weight, down_weight):
    ep_count = lax.axis_size("ep")
    tok_rows, width = tokens.shape
    slots = chosen.shape[1]
    per_source = slots // ep_count
    rows = ep_count * per_source
    units = gate_weight.shape[2]
    swap = [(0, 1), (1, 0)]

    order = jnp.arange(slots, dtype=jnp.int32)[None, :]
    (spread,) = call(
        lambda *refs: prep_kernel(per_source, *refs), [VMEM],
        (jax.ShapeDtypeStruct((slots, slots), jnp.bfloat16),), 10**10, (order % per_source,),
    )
    parts, codes, stride = [chosen], [0], ep_count
    while stride > 1:
        ids = jnp.concatenate(parts, axis=0)
        radix = 4 if stride % 4 == 0 else 2
        stride //= radix
        codes = [k * stride + c for k in range(radix) for c in codes]
        first = stride * radix == ep_count
        parts = gather_round(ids, stride, radix, ep_count)
        if first:
            parts, spread = lax.optimization_barrier((parts, spread))

    outgoing, row = call(
        pick_kernel, [VMEM] * (4 + len(parts)),
        (
            jax.ShapeDtypeStruct((rows, width), tokens.dtype),
            jax.ShapeDtypeStruct((1, slots), jnp.int32),
        ),
        200 * rows * tok_rows * width,
        (order // per_source, jnp.array(codes, jnp.int32)[:, None], spread, tokens, *parts),
        [pltpu.VMEM((ep_count, slots), jnp.int32)],
    )
    arrived = lax.all_to_all(
        outgoing.reshape(ep_count, per_source, width), "ep", split_axis=0, concat_axis=0, tiled=True
    ).reshape(rows, width)
    other = lax.ppermute(arrived, "tp", swap)
    pre = jax.ShapeDtypeStruct((rows, units), jnp.float32)
    product = 2 * rows * width * units
    gate_pre, up_pre = call(
        first_kernel, [VMEM] * 4, (pre, pre), 2 * product,
        (arrived, gate_weight, up_weight, down_weight),
    )
    hidden, sent = call(
        second_kernel, [VMEM] * 7,
        (
            jax.ShapeDtypeStruct((rows, units), jnp.bfloat16),
            jax.ShapeDtypeStruct((rows, width), jnp.bfloat16),
        ),
        3 * product,
        (other, gate_pre, up_pre, gate_weight, up_weight, down_weight, gate_score),
    )
    got = lax.ppermute(sent, "tp", swap)
    (kept,) = call(
        third_kernel, [VMEM] * 2,
        (jax.ShapeDtypeStruct((rows, width), jnp.float32),), product,
        (hidden, down_weight),
    )
    weighted = (kept + got.astype(jnp.float32)).astype(jnp.bfloat16)
    returned = lax.all_to_all(
        weighted.reshape(ep_count, per_source, width), "ep", split_axis=0, concat_axis=0, tiled=True
    ).reshape(rows, width)
    (mixed_out,) = call(
        mix_kernel, [VMEM] * 2, (jax.ShapeDtypeStruct((tok_rows, width), jnp.bfloat16),),
        2 * rows * tok_rows * width, (row, returned),
    )
    return mixed_out


def solution(mesh):
    in_specs = (
        P("ep", "tp"),
        P("ep", None),
        P("ep", None),
        P("ep", None, "tp"),
        P("ep", None, "tp"),
        P("ep", "tp", None),
    )
    out_specs = P("ep", "tp")
    return jax.shard_map(layer, mesh=mesh, in_specs=in_specs, out_specs=out_specs, check_vma=False)
```

```python
import jax
import jax.numpy as jnp
from jax import lax
from jax.experimental import pallas as pl
from jax.experimental.pallas import tpu as pltpu
from jax.sharding import PartitionSpec as P


VMEM = pl.BlockSpec(memory_space=pltpu.VMEM)
HBM = pl.BlockSpec(memory_space=pltpu.HBM)
MIB = 1 << 20


def nbytes(x):
    return x.size * x.dtype.itemsize


def call(body, in_specs, outs, flops, args, scratch=(), out_spec=VMEM):
    held = sum(nbytes(x) for x in outs)
    held += sum(nbytes(x) for x, spec in zip(args, in_specs) if spec is VMEM)
    return pl.pallas_call(
        body,
        out_shape=outs,
        in_specs=in_specs,
        out_specs=tuple(out_spec for _ in outs),
        scratch_shapes=scratch,
        cost_estimate=pl.CostEstimate(flops=flops, bytes_accessed=held, transcendentals=0),
        compiler_params=pltpu.CompilerParams(
            vmem_limit_bytes=min(held + 6 * MIB, 60 * MIB)
        ),
    )(*args)


def dot(a, b):
    return jnp.dot(a, b, preferred_element_type=jnp.float32)


def half(which, width):
    return pl.ds(pl.multiple_of(which * width, width), width)


def prep_kernel(per_source, within_ref, spread_ref):
    slots = within_ref.shape[1]
    column = lax.broadcasted_iota(jnp.int32, (slots, slots), 0)
    hit = column == lax.axis_index("ep") * per_source + within_ref[...]
    spread_ref[...] = hit.astype(jnp.float32).astype(jnp.bfloat16)


def pick_kernel(expert_ref, code_ref, spread_ref, tokens_ref, *refs):
    parts, (out_ref, row_ref, ids_ref) = refs[:-3], refs[-3:]
    me = lax.axis_index("ep")
    tok_rows, slots = tokens_ref.shape[0], spread_ref.shape[0]
    step = parts[0].shape[0]
    count = step * len(parts)
    for j, part in enumerate(parts):
        ids_ref[pl.ds(j * step, step), :] = part[...]
    local = ids_ref[...] - me * tok_rows
    low, high = local & 127, local >> 7
    both = jnp.concatenate([high, low], axis=0).astype(jnp.float32).astype(jnp.bfloat16)
    mine = dot(both, spread_ref[...])
    mine = mine[:count] * 128.0 + mine[count:]
    ours = code_ref[...] == (expert_ref[...] ^ me)
    row = jnp.sum(jnp.where(ours, mine, 0.0), axis=0, keepdims=True).astype(jnp.int32)
    row_ref[...] = row
    selector = lax.broadcasted_iota(jnp.int32, (tok_rows, slots), 0) == row
    out_ref[...] = lax.dot_general(
        selector.astype(jnp.float32).astype(jnp.bfloat16), tokens_ref[...],
        (((0,), (0,)), ((), ())), preferred_element_type=jnp.float32,
    ).astype(jnp.bfloat16)


def first_kernel(own_ref, gate_w, up_w, down_w, gate_ref, up_ref):
    del down_w
    mine = half(lax.axis_index("tp"), own_ref.shape[1])
    gate_ref[...] = dot(own_ref[...], gate_w[0, mine, :])
    up_ref[...] = dot(own_ref[...], up_w[0, mine, :])


def second_kernel(
    other_ref, gate_ref, up_ref, gate_w, up_w, down_w, score_ref, hidden_ref, send_ref
):
    theirs = half(1 - lax.axis_index("tp"), other_ref.shape[1])
    rows, units = gate_ref.shape
    tile = 512 if units % 512 == 0 else units
    score = jnp.transpose(jnp.broadcast_to(score_ref[...], (128, rows)))
    score = jnp.concatenate([score] * (tile // 128), axis=1)
    for start in range(0, units, tile):
        c = pl.ds(start, tile)
        gate_pre = gate_ref[:, c] + dot(other_ref[...], gate_w[0, theirs, c])
        up_pre = up_ref[:, c] + dot(other_ref[...], up_w[0, theirs, c])
        hidden = gate_pre / (1.0 + jnp.exp(-gate_pre)) * (up_pre * score)
        hidden_ref[:, c] = hidden.astype(jnp.bfloat16)
    send_ref[...] = dot(hidden_ref[...], down_w[0, :, theirs]).astype(jnp.bfloat16)


def third_kernel(hidden_ref, down_w, keep_ref):
    keep_ref[...] = dot(hidden_ref[...], down_w[0, :, half(lax.axis_index("tp"), keep_ref.shape[1])])


def join_kernel(keep_ref, got_ref, out_ref):
    out_ref[...] = (keep_ref[...] + got_ref[...].astype(jnp.float32)).astype(jnp.bfloat16)


def mix_kernel(row_ref, returned_ref, out_hbm, mixed_ref, sems):
    tok_rows, width = out_hbm.shape
    shape = (tok_rows, row_ref.shape[1])
    selector = lax.broadcasted_iota(jnp.int32, shape, 0) == row_ref[...]
    selector = selector.astype(jnp.float32).astype(jnp.bfloat16)
    copies = []
    for j in range(2):
        at = pl.ds(j * width // 2, width // 2)
        mixed_ref[:, at] = dot(selector, returned_ref[:, at]).astype(mixed_ref.dtype)
        copies.append(pltpu.make_async_copy(mixed_ref.at[:, at], out_hbm.at[:, at], sems.at[j]))
        copies[-1].start()
    for copy in copies:
        copy.wait()


def gather_round(value, stride, radix, count):
    parts = [value]
    for k in range(1, radix):
        parts.append(lax.ppermute(value, "ep", [(e, e ^ (k * stride)) for e in range(count)]))
    return parts


def layer(tokens, chosen, gate_score, gate_weight, up_weight, down_weight):
    ep_count = lax.axis_size("ep")
    tok_rows, width = tokens.shape
    slots = chosen.shape[1]
    per_source = slots // ep_count
    rows = ep_count * per_source
    units = gate_weight.shape[2]
    swap = [(0, 1), (1, 0)]

    order = jnp.arange(slots, dtype=jnp.int32)[None, :]
    (spread,) = call(
        lambda *refs: prep_kernel(per_source, *refs), [VMEM],
        (jax.ShapeDtypeStruct((slots, slots), jnp.bfloat16),), 10**10, (order % per_source,),
    )
    parts, codes, stride = [chosen], [0], ep_count
    while stride > 1:
        ids = jnp.concatenate(parts, axis=0)
        radix = 4 if stride % 4 == 0 else 2
        stride //= radix
        codes = [k * stride + c for k in range(radix) for c in codes]
        first = stride * radix == ep_count
        parts = gather_round(ids, stride, radix, ep_count)
        if first:
            parts, spread = lax.optimization_barrier((parts, spread))

    outgoing, row = call(
        pick_kernel, [VMEM] * (4 + len(parts)),
        (
            jax.ShapeDtypeStruct((rows, width), tokens.dtype),
            jax.ShapeDtypeStruct((1, slots), jnp.int32),
        ),
        200 * rows * tok_rows * width,
        (order // per_source, jnp.array(codes, jnp.int32)[:, None], spread, tokens, *parts),
        [pltpu.VMEM((ep_count, slots), jnp.int32)],
    )
    arrived = lax.all_to_all(
        outgoing.reshape(ep_count, per_source, width), "ep", split_axis=0, concat_axis=0, tiled=True
    ).reshape(rows, width)
    other = lax.ppermute(arrived, "tp", swap)
    pre = jax.ShapeDtypeStruct((rows, units), jnp.float32)
    product = 2 * rows * width * units
    gate_pre, up_pre = call(
        first_kernel, [VMEM] * 4, (pre, pre), 2 * product,
        (arrived, gate_weight, up_weight, down_weight),
    )
    hidden, sent = call(
        second_kernel, [VMEM] * 7,
        (
            jax.ShapeDtypeStruct((rows, units), jnp.bfloat16),
            jax.ShapeDtypeStruct((rows, width), jnp.bfloat16),
        ),
        3 * product,
        (other, gate_pre, up_pre, gate_weight, up_weight, down_weight, gate_score),
    )
    got = lax.ppermute(sent, "tp", swap)
    (kept,) = call(
        third_kernel, [VMEM] * 2,
        (jax.ShapeDtypeStruct((rows, width), jnp.float32),), product,
        (hidden, down_weight),
    )
    (weighted,) = call(
        join_kernel, [VMEM] * 2, (jax.ShapeDtypeStruct((rows, width), jnp.bfloat16),),
        rows * width, (kept, got),
    )
    returned = lax.all_to_all(
        weighted.reshape(ep_count, per_source, width), "ep", split_axis=0, concat_axis=0, tiled=True
    ).reshape(rows, width)
    (mixed_out,) = call(
        mix_kernel, [VMEM] * 2, (jax.ShapeDtypeStruct((tok_rows, width), jnp.bfloat16),),
        2 * rows * tok_rows * width, (row, returned),
        [pltpu.VMEM((tok_rows, width), jnp.bfloat16), pltpu.SemaphoreType.DMA((2,))], HBM,
    )
    return mixed_out


def solution(mesh):
    in_specs = (
        P("ep", "tp"),
        P("ep", None),
        P("ep", None),
        P("ep", None, "tp"),
        P("ep", None, "tp"),
        P("ep", "tp", None),
    )
    out_specs = P("ep", "tp")
    return jax.shard_map(layer, mesh=mesh, in_specs=in_specs, out_specs=out_specs, check_vma=False)
```

```python
import jax
import jax.numpy as jnp
from jax import lax
from jax.experimental import pallas as pl
from jax.experimental.pallas import tpu as pltpu
from jax.sharding import PartitionSpec as P


VMEM = pl.BlockSpec(memory_space=pltpu.VMEM)
HBM = pl.BlockSpec(memory_space=pltpu.HBM)
MIB = 1 << 20


def nbytes(x):
    return x.size * x.dtype.itemsize


def call(body, in_specs, outs, flops, args, scratch=(), out_spec=VMEM):
    held = sum(nbytes(x) for x in outs)
    held += sum(nbytes(x) for x, spec in zip(args, in_specs) if spec is VMEM)
    return pl.pallas_call(
        body,
        out_shape=outs,
        in_specs=in_specs,
        out_specs=tuple(out_spec for _ in outs),
        scratch_shapes=scratch,
        cost_estimate=pl.CostEstimate(flops=flops, bytes_accessed=held, transcendentals=0),
        compiler_params=pltpu.CompilerParams(
            vmem_limit_bytes=min(held + 6 * MIB, 60 * MIB)
        ),
    )(*args)


def dot(a, b):
    return jnp.dot(a, b, preferred_element_type=jnp.float32)


def half(which, width):
    return pl.ds(pl.multiple_of(which * width, width), width)


def prep_kernel(per_source, within_ref, spread_ref):
    slots = within_ref.shape[1]
    column = lax.broadcasted_iota(jnp.int32, (slots, slots), 0)
    hit = column == lax.axis_index("ep") * per_source + within_ref[...]
    spread_ref[...] = hit.astype(jnp.float32).astype(jnp.bfloat16)


def pick_kernel(expert_ref, code_ref, spread_ref, tokens_ref, *refs):
    parts, (out_ref, row_ref, ids_ref) = refs[:-3], refs[-3:]
    me = lax.axis_index("ep")
    tok_rows, slots = tokens_ref.shape[0], spread_ref.shape[0]
    step = parts[0].shape[0]
    count = step * len(parts)
    for j, part in enumerate(parts):
        ids_ref[pl.ds(j * step, step), :] = part[...]
    local = ids_ref[...] - me * tok_rows
    low, high = local & 127, local >> 7
    both = jnp.concatenate([high, low], axis=0).astype(jnp.float32).astype(jnp.bfloat16)
    mine = dot(both, spread_ref[...])
    mine = mine[:count] * 128.0 + mine[count:]
    ours = code_ref[...] == (expert_ref[...] ^ me)
    row = jnp.sum(jnp.where(ours, mine, 0.0), axis=0, keepdims=True).astype(jnp.int32)
    row_ref[...] = row
    selector = lax.broadcasted_iota(jnp.int32, (tok_rows, slots), 0) == row
    out_ref[...] = lax.dot_general(
        selector.astype(jnp.float32).astype(jnp.bfloat16), tokens_ref[...],
        (((0,), (0,)), ((), ())), preferred_element_type=jnp.float32,
    ).astype(jnp.bfloat16)


def first_kernel(own_ref, gate_w, up_w, down_w, gate_ref, up_ref):
    del down_w
    mine = half(lax.axis_index("tp"), own_ref.shape[1])
    gate_ref[...] = dot(own_ref[...], gate_w[0, mine, :])
    up_ref[...] = dot(own_ref[...], up_w[0, mine, :])


def second_kernel(
    other_ref, gate_ref, up_ref, gate_w, up_w, down_w, score_ref, hidden_ref, send_ref
):
    theirs = half(1 - lax.axis_index("tp"), other_ref.shape[1])
    rows, units = gate_ref.shape
    tile = 512 if units % 512 == 0 else units
    score = jnp.transpose(jnp.broadcast_to(score_ref[...], (128, rows)))
    score = jnp.concatenate([score] * (tile // 128), axis=1)
    for start in range(0, units, tile):
        c = pl.ds(start, tile)
        gate_pre = gate_ref[:, c] + dot(other_ref[...], gate_w[0, theirs, c])
        up_pre = up_ref[:, c] + dot(other_ref[...], up_w[0, theirs, c])
        hidden = gate_pre / (1.0 + jnp.exp(-gate_pre)) * (up_pre * score)
        hidden_ref[:, c] = hidden.astype(jnp.bfloat16)
    send_ref[...] = dot(hidden_ref[...], down_w[0, :, theirs]).astype(jnp.bfloat16)


def third_kernel(hidden_ref, down_w, keep_ref):
    keep_ref[...] = dot(hidden_ref[...], down_w[0, :, half(lax.axis_index("tp"), keep_ref.shape[1])])


def join_kernel(keep_ref, got_ref, out_ref):
    out_ref[...] = (keep_ref[...] + got_ref[...].astype(jnp.float32)).astype(jnp.bfloat16)


def mix_kernel(row_ref, returned_ref, out_hbm, mixed_ref, sems):
    tok_rows, width = out_hbm.shape
    shape = (tok_rows, row_ref.shape[1])
    selector = lax.broadcasted_iota(jnp.int32, shape, 0) == row_ref[...]
    selector = selector.astype(jnp.float32).astype(jnp.bfloat16)
    copies = []
    for j in range(4):
        at = pl.ds(j * width // 4, width // 4)
        mixed_ref[:, at] = dot(selector, returned_ref[:, at]).astype(mixed_ref.dtype)
        copies.append(pltpu.make_async_copy(mixed_ref.at[:, at], out_hbm.at[:, at], sems.at[j]))
        copies[-1].start()
    for copy in copies:
        copy.wait()


def gather_round(value, stride, radix, count):
    parts = [value]
    for k in range(1, radix):
        parts.append(lax.ppermute(value, "ep", [(e, e ^ (k * stride)) for e in range(count)]))
    return parts


def layer(tokens, chosen, gate_score, gate_weight, up_weight, down_weight):
    ep_count = lax.axis_size("ep")
    tok_rows, width = tokens.shape
    slots = chosen.shape[1]
    per_source = slots // ep_count
    rows = ep_count * per_source
    units = gate_weight.shape[2]
    swap = [(0, 1), (1, 0)]

    order = jnp.arange(slots, dtype=jnp.int32)[None, :]
    (spread,) = call(
        lambda *refs: prep_kernel(per_source, *refs), [VMEM],
        (jax.ShapeDtypeStruct((slots, slots), jnp.bfloat16),), 10**10, (order % per_source,),
    )
    parts, codes, stride = [chosen], [0], ep_count
    while stride > 1:
        ids = jnp.concatenate(parts, axis=0)
        radix = 4 if stride % 4 == 0 else 2
        stride //= radix
        codes = [k * stride + c for k in range(radix) for c in codes]
        first = stride * radix == ep_count
        parts = gather_round(ids, stride, radix, ep_count)
        if first:
            parts, spread = lax.optimization_barrier((parts, spread))

    outgoing, row = call(
        pick_kernel, [VMEM] * (4 + len(parts)),
        (
            jax.ShapeDtypeStruct((rows, width), tokens.dtype),
            jax.ShapeDtypeStruct((1, slots), jnp.int32),
        ),
        200 * rows * tok_rows * width,
        (order // per_source, jnp.array(codes, jnp.int32)[:, None], spread, tokens, *parts),
        [pltpu.VMEM((ep_count, slots), jnp.int32)],
    )
    arrived = lax.all_to_all(
        outgoing.reshape(ep_count, per_source, width), "ep", split_axis=0, concat_axis=0, tiled=True
    ).reshape(rows, width)
    other = lax.ppermute(arrived, "tp", swap)
    pre = jax.ShapeDtypeStruct((rows, units), jnp.float32)
    product = 2 * rows * width * units
    gate_pre, up_pre = call(
        first_kernel, [VMEM] * 4, (pre, pre), 2 * product,
        (arrived, gate_weight, up_weight, down_weight),
    )
    hidden, sent = call(
        second_kernel, [VMEM] * 7,
        (
            jax.ShapeDtypeStruct((rows, units), jnp.bfloat16),
            jax.ShapeDtypeStruct((rows, width), jnp.bfloat16),
        ),
        3 * product,
        (other, gate_pre, up_pre, gate_weight, up_weight, down_weight, gate_score),
    )
    got = lax.ppermute(sent, "tp", swap)
    (kept,) = call(
        third_kernel, [VMEM] * 2,
        (jax.ShapeDtypeStruct((rows, width), jnp.float32),), product,
        (hidden, down_weight),
    )
    (weighted,) = call(
        join_kernel, [VMEM] * 2, (jax.ShapeDtypeStruct((rows, width), jnp.bfloat16),),
        rows * width, (kept, got),
    )
    returned = lax.all_to_all(
        weighted.reshape(ep_count, per_source, width), "ep", split_axis=0, concat_axis=0, tiled=True
    ).reshape(rows, width)
    (mixed_out,) = call(
        mix_kernel, [VMEM] * 2, (jax.ShapeDtypeStruct((tok_rows, width), jnp.bfloat16),),
        2 * rows * tok_rows * width, (row, returned),
        [pltpu.VMEM((tok_rows, width), jnp.bfloat16), pltpu.SemaphoreType.DMA((4,))], HBM,
    )
    return mixed_out


def solution(mesh):
    in_specs = (
        P("ep", "tp"),
        P("ep", None),
        P("ep", None),
        P("ep", None, "tp"),
        P("ep", None, "tp"),
        P("ep", "tp", None),
    )
    out_specs = P("ep", "tp")
    return jax.shard_map(layer, mesh=mesh, in_specs=in_specs, out_specs=out_specs, check_vma=False)
```

```python
import jax
import jax.numpy as jnp
from jax import lax
from jax.experimental import pallas as pl
from jax.experimental.pallas import tpu as pltpu
from jax.sharding import PartitionSpec as P


VMEM = pl.BlockSpec(memory_space=pltpu.VMEM)
HBM = pl.BlockSpec(memory_space=pltpu.HBM)
MIB = 1 << 20


def nbytes(x):
    return x.size * x.dtype.itemsize


def call(body, in_specs, outs, flops, args, scratch=(), out_spec=VMEM):
    held = sum(nbytes(x) for x in outs)
    held += sum(nbytes(x) for x, spec in zip(args, in_specs) if spec is VMEM)
    return pl.pallas_call(
        body,
        out_shape=outs,
        in_specs=in_specs,
        out_specs=tuple(out_spec for _ in outs),
        scratch_shapes=scratch,
        cost_estimate=pl.CostEstimate(flops=flops, bytes_accessed=held, transcendentals=0),
        compiler_params=pltpu.CompilerParams(
            vmem_limit_bytes=min(held + 6 * MIB, 60 * MIB)
        ),
    )(*args)


def dot(a, b):
    return jnp.dot(a, b, preferred_element_type=jnp.float32)


def half(which, width):
    return pl.ds(pl.multiple_of(which * width, width), width)


def prep_kernel(per_source, within_ref, spread_ref):
    slots = within_ref.shape[1]
    column = lax.broadcasted_iota(jnp.int32, (slots, slots), 0)
    hit = column == lax.axis_index("ep") * per_source + within_ref[...]
    spread_ref[...] = hit.astype(jnp.float32).astype(jnp.bfloat16)


def pick_kernel(expert_ref, code_ref, spread_ref, tokens_ref, *refs):
    parts, (out_ref, selector_ref, ids_ref) = refs[:-3], refs[-3:]
    me = lax.axis_index("ep")
    tok_rows, slots = tokens_ref.shape[0], spread_ref.shape[0]
    step = parts[0].shape[0]
    count = step * len(parts)
    for j, part in enumerate(parts):
        ids_ref[pl.ds(j * step, step), :] = part[...]
    local = ids_ref[...] - me * tok_rows
    if tok_rows <= 256:
        mine = dot(local.astype(jnp.float32).astype(jnp.bfloat16), spread_ref[...])
    else:
        low, high = local & 127, local >> 7
        both = jnp.concatenate([high, low], axis=0).astype(jnp.float32).astype(jnp.bfloat16)
        mine = dot(both, spread_ref[...])
        mine = mine[:count] * 128.0 + mine[count:]
    ours = code_ref[...] == (expert_ref[...] ^ me)
    row = jnp.sum(jnp.where(ours, mine, 0.0), axis=0, keepdims=True).astype(jnp.int32)
    selector = lax.broadcasted_iota(jnp.int32, (tok_rows, slots), 0) == row
    selector = selector.astype(jnp.float32).astype(jnp.bfloat16)
    selector_ref[...] = selector
    out_ref[...] = lax.dot_general(
        selector, tokens_ref[...], (((0,), (0,)), ((), ())), preferred_element_type=jnp.float32
    ).astype(jnp.bfloat16)


def first_kernel(own_ref, gate_w, up_w, down_w, gate_ref, up_ref):
    del down_w
    mine = half(lax.axis_index("tp"), own_ref.shape[1])
    gate_ref[...] = dot(own_ref[...], gate_w[0, mine, :])
    up_ref[...] = dot(own_ref[...], up_w[0, mine, :])


def second_kernel(
    other_ref, gate_ref, up_ref, gate_w, up_w, down_w, score_ref, hidden_ref, send_ref
):
    theirs = half(1 - lax.axis_index("tp"), other_ref.shape[1])
    rows, units = gate_ref.shape
    tile = 512 if units % 512 == 0 else units
    score = jnp.transpose(jnp.broadcast_to(score_ref[...], (128, rows)))
    score = jnp.concatenate([score] * (tile // 128), axis=1)
    for start in range(0, units, tile):
        c = pl.ds(start, tile)
        gate_pre = gate_ref[:, c] + dot(other_ref[...], gate_w[0, theirs, c])
        up_pre = up_ref[:, c] + dot(other_ref[...], up_w[0, theirs, c])
        hidden = gate_pre / (1.0 + jnp.exp(-gate_pre)) * (up_pre * score)
        hidden_ref[:, c] = hidden.astype(jnp.bfloat16)
    send_ref[...] = dot(hidden_ref[...], down_w[0, :, theirs]).astype(jnp.bfloat16)


def third_kernel(hidden_ref, down_w, keep_ref):
    keep_ref[...] = dot(hidden_ref[...], down_w[0, :, half(lax.axis_index("tp"), keep_ref.shape[1])])


def join_kernel(keep_ref, got_ref, out_ref):
    out_ref[...] = (keep_ref[...] + got_ref[...].astype(jnp.float32)).astype(jnp.bfloat16)


def mix_kernel(selector_ref, returned_ref, out_hbm, mixed_ref, sems):
    width = out_hbm.shape[1]
    copies = []
    for j in range(2):
        at = pl.ds(j * width // 2, width // 2)
        mixed_ref[:, at] = dot(selector_ref[...], returned_ref[:, at]).astype(mixed_ref.dtype)
        copies.append(pltpu.make_async_copy(mixed_ref.at[:, at], out_hbm.at[:, at], sems.at[j]))
        copies[-1].start()
    for copy in copies:
        copy.wait()


def gather_round(value, stride, radix, count):
    parts = [value]
    for k in range(1, radix):
        parts.append(lax.ppermute(value, "ep", [(e, e ^ (k * stride)) for e in range(count)]))
    return parts


def layer(tokens, chosen, gate_score, gate_weight, up_weight, down_weight):
    ep_count = lax.axis_size("ep")
    tok_rows, width = tokens.shape
    slots = chosen.shape[1]
    per_source = slots // ep_count
    rows = ep_count * per_source
    units = gate_weight.shape[2]
    swap = [(0, 1), (1, 0)]

    order = jnp.arange(slots, dtype=jnp.int32)[None, :]
    (spread,) = call(
        lambda *refs: prep_kernel(per_source, *refs), [VMEM],
        (jax.ShapeDtypeStruct((slots, slots), jnp.bfloat16),), 10**10, (order % per_source,),
    )
    parts, codes, stride = [chosen], [0], ep_count
    while stride > 1:
        ids = jnp.concatenate(parts, axis=0)
        radix = 4 if stride % 4 == 0 else 2
        stride //= radix
        codes = [k * stride + c for k in range(radix) for c in codes]
        first = stride * radix == ep_count
        parts = gather_round(ids, stride, radix, ep_count)
        if first:
            parts, spread = lax.optimization_barrier((parts, spread))

    outgoing, selector = call(
        pick_kernel, [VMEM] * (4 + len(parts)),
        (
            jax.ShapeDtypeStruct((rows, width), tokens.dtype),
            jax.ShapeDtypeStruct((tok_rows, slots), jnp.bfloat16),
        ),
        200 * rows * tok_rows * width,
        (order // per_source, jnp.array(codes, jnp.int32)[:, None], spread, tokens, *parts),
        [pltpu.VMEM((ep_count, slots), jnp.int32)],
    )
    arrived = lax.all_to_all(
        outgoing.reshape(ep_count, per_source, width), "ep", split_axis=0, concat_axis=0, tiled=True
    ).reshape(rows, width)
    other = lax.ppermute(arrived, "tp", swap)
    pre = jax.ShapeDtypeStruct((rows, units), jnp.float32)
    product = 2 * rows * width * units
    gate_pre, up_pre = call(
        first_kernel, [VMEM] * 4, (pre, pre), 2 * product,
        (arrived, gate_weight, up_weight, down_weight),
    )
    hidden, sent = call(
        second_kernel, [VMEM] * 7,
        (
            jax.ShapeDtypeStruct((rows, units), jnp.bfloat16),
            jax.ShapeDtypeStruct((rows, width), jnp.bfloat16),
        ),
        3 * product,
        (other, gate_pre, up_pre, gate_weight, up_weight, down_weight, gate_score),
    )
    got = lax.ppermute(sent, "tp", swap)
    (kept,) = call(
        third_kernel, [VMEM] * 2,
        (jax.ShapeDtypeStruct((rows, width), jnp.float32),), product,
        (hidden, down_weight),
    )
    (weighted,) = call(
        join_kernel, [VMEM] * 2, (jax.ShapeDtypeStruct((rows, width), jnp.bfloat16),),
        rows * width, (kept, got),
    )
    returned = lax.all_to_all(
        weighted.reshape(ep_count, per_source, width), "ep", split_axis=0, concat_axis=0, tiled=True
    ).reshape(rows, width)
    (mixed_out,) = call(
        mix_kernel, [VMEM] * 2, (jax.ShapeDtypeStruct((tok_rows, width), jnp.bfloat16),),
        2 * rows * tok_rows * width, (selector, returned),
        [pltpu.VMEM((tok_rows, width), jnp.bfloat16), pltpu.SemaphoreType.DMA((2,))], HBM,
    )
    return mixed_out


def solution(mesh):
    in_specs = (
        P("ep", "tp"),
        P("ep", None),
        P("ep", None),
        P("ep", None, "tp"),
        P("ep", None, "tp"),
        P("ep", "tp", None),
    )
    out_specs = P("ep", "tp")
    return jax.shard_map(layer, mesh=mesh, in_specs=in_specs, out_specs=out_specs, check_vma=False)
```
